32 devices in a mesh: rep: 4 (over y, x), fs: 2 (over core), tp: 4 (over z).
Axes of the slice: x: 2, y: 2, z: 4, core: 2. Of those that a mesh axis runs over, the one named last changes fastest.
Arguments:
- layer_input: bfloat16 [10240, 2048], P(('rep', 'fs'), 'tp'), may hold values from -6 to 6
- cotangent: bfloat16 [10240, 2048], P(('rep', 'fs'), 'tp'), may hold values from -8 to 8
- gate_pre: bfloat16 [10240, 3072], P('rep', 'fs'), may hold values from -8 to 8
- up_pre: bfloat16 [10240, 3072], P('rep', 'fs'), may hold values from -6 to 6
- gate_weight: bfloat16 [2048, 3072], P('tp', 'fs'), may hold values from -0.125 to 0.125
- up_weight: bfloat16 [2048, 3072], P('tp', 'fs'), may hold values from -0.125 to 0.125
- down_weight: bfloat16 [3072, 2048], P('fs', 'tp'), may hold values from -0.109375 to 0.109375
Outputs:
- input_grad: bfloat16 [10240, 2048], P(('rep', 'fs'), 'tp')
- gate_grad: float32 [2048, 3072], P('tp', 'fs')
- up_grad: float32 [2048, 3072], P('tp', 'fs')
- down_grad: float32 [3072, 2048], P('fs', 'tp')
- gate_rows_sq: float32 [2048], P('tp')
- up_rows_sq: float32 [2048], P('tp')
- down_rows_sq: float32 [3072], P('fs')
The draws below stay inside these ranges and needn't reach their ends.
All inputs are finite; a program needn't handle non-finite values.
Results may differ from the reference program's by a relative error of at most 0.019.
Values may be sent and summed in bfloat16 or wider, within the bound.
A program may use at most 128 MiB of HBM per device.

```python
import math
import jax
import jax.numpy as jnp
from jax import lax

D = 2048
FF = 3072
TOKENS = 10240
N_FS = 2


def with_spikes(values, own_key, source, target, blocks, factor):
    owner, partner = [(jnp.arange(values.shape[position]) // (values.shape[position] // blocks)).reshape([-1 if axis == position else 1 for axis in range(values.ndim)]) for position in (source, target)]
    chosen = jax.random.permutation(own_key, blocks)[partner]
    strong = (owner == chosen) | (owner == (partner + blocks // 2) % blocks)
    return jnp.where(strong, factor * values, values)


def steps_of(key, shape, pieces, smallest, top_value):
    loudness, own = 1.0, jax.random.fold_in(key, 6)
    for dim, blocks in pieces:
        heights = jnp.exp(jax.random.uniform(jax.random.fold_in(own, dim), (blocks,), jnp.float32, smallest / len(pieces), top_value / len(pieces)))
        loudness = loudness * jnp.repeat(heights, shape[dim] // blocks).reshape([-1 if axis == dim else 1 for axis in range(len(shape))])
    return loudness


def bell_draw(key, shape, deviation, most, shards=(), held_as=jnp.bfloat16):
    drawn = deviation * jax.random.normal(key, shape, jnp.float32)
    if shards:
        drawn = drawn * steps_of(key, shape, shards, -0.22, 0.18)
    return jnp.clip(drawn, -most, most).astype(held_as)


def heavy_noise(stream_key, extent, spread, limit, shards, heavy, kind=jnp.bfloat16):
    drawn = spread * jax.random.normal(stream_key, extent, jnp.float32)
    if shards:
        drawn = drawn * steps_of(stream_key, extent, shards, -0.22, 0.18)
    return jnp.clip(with_spikes(drawn, jax.random.fold_in(stream_key, 3), *heavy), -limit, limit).astype(kind)


def setup_inputs(seed: int = 0) -> dict:
    seeds = jax.random.split(jax.random.key(seed), 8)
    return {
        "layer_input": bell_draw(seeds[0], (TOKENS, D), 1.0, 6.0, ((0, 8), (1, 4))),
        "cotangent": heavy_noise(seeds[1], (TOKENS, D), 1.0, 8.0, ((0, 8), (1, 4)), (0, 1, 8, 2.0)),
        "gate_pre": bell_draw(seeds[2], (TOKENS, FF), 1.5, 8.0, ((0, 4), (1, 2))),
        "up_pre": bell_draw(seeds[3], (TOKENS, FF), 1.0, 6.0, ((0, 4), (1, 2))),
        "gate_weight": bell_draw(seeds[4], (D, FF), D ** -0.5, 0.125, ((0, 4), (1, 2))),
        "up_weight": bell_draw(seeds[5], (D, FF), D ** -0.5, 0.125, ((0, 4), (1, 2))),
        "down_weight": bell_draw(seeds[6], (FF, D), FF ** -0.5, 0.109375, ((0, 2), (1, 4))),
    }


def contract_rows(left_side, right_side):
    return lax.dot_general(left_side, right_side, (((0,), (0,)), ((), ())), preferred_element_type=jnp.float32)

def contract_cols(left_side, right_side):
    return lax.dot_general(left_side, right_side, (((1,), (1,)), ((), ())), preferred_element_type=jnp.float32)

def reference(layer_input, cotangent, gate_pre, up_pre, gate_weight, up_weight, down_weight):
    hidden_grad = contract_cols(cotangent, down_weight)
    gate_value = gate_pre.astype(jnp.float32)
    up_value = up_pre.astype(jnp.float32)
    sigmoid_gate = jax.nn.sigmoid(gate_value)
    activated = gate_value * sigmoid_gate
    hidden = (activated * up_value).astype(jnp.bfloat16)
    gate_delta = (hidden_grad * up_value * sigmoid_gate * (1.0 + gate_value * (1.0 - sigmoid_gate))).astype(jnp.bfloat16)
    up_delta = (hidden_grad * activated).astype(jnp.bfloat16)
    block = FF // N_FS
    input_sum = jnp.zeros((TOKENS, D), jnp.float32)
    for block_index in range(N_FS):
        first = block_index * block
        partial_sum = contract_cols(gate_delta[:, first:first + block], gate_weight[:, first:first + block])
        partial_sum = partial_sum + contract_cols(up_delta[:, first:first + block], up_weight[:, first:first + block])
        rounded = lax.optimization_barrier(partial_sum.astype(jnp.bfloat16))
        input_sum = input_sum + rounded.astype(jnp.float32)
    input_grad = input_sum.astype(jnp.bfloat16)
    grad_scale = 1.0 / math.sqrt(TOKENS)
    gate_grad = contract_rows(layer_input, gate_delta) * grad_scale
    up_grad = contract_rows(layer_input, up_delta) * grad_scale
    down_grad = contract_rows(hidden, cotangent) * grad_scale
    gate_rows_sq = lax.optimization_barrier(jnp.sum(gate_grad * gate_grad, axis=1))
    up_rows_sq = lax.optimization_barrier(jnp.sum(up_grad * up_grad, axis=1))
    down_rows_sq = lax.optimization_barrier(jnp.sum(down_grad * down_grad, axis=1))
    return (input_grad, gate_grad, up_grad, down_grad, gate_rows_sq, up_rows_sq, down_rows_sq)
```

```python
import functools
import math

import jax
import jax.numpy as jnp
from jax import lax
from jax.experimental import pallas as pl
from jax.experimental.pallas import tpu as pltpu
from jax.sharding import PartitionSpec as P

MESH = pl.DeviceIdType.MESH
F32 = jnp.float32
BF16 = jnp.bfloat16


def dot(left_side, right_side, left_dim, right_dim):
    return lax.dot_general(
        left_side,
        right_side,
        (((left_dim,), (right_dim,)), ((), ())),
        preferred_element_type=F32,
    )


def shift(value, axis, by):
    size = lax.axis_size(axis)
    return lax.ppermute(value, axis, [(i, (i + by) % size) for i in range(size)])


def sum_small(value, axis):
    total = value
    for by in range(1, lax.axis_size(axis)):
        total = total + shift(value, axis, by)
    return total


class Sum:
    def __init__(self, acc, out, row, rows, cols, swap, stage, first, second, done, sems, at):
        self.acc, self.out, self.cols, self.sems, self.at = acc, out, cols, sems, at
        self.stage, self.first, self.second, self.done = stage, first, second, done
        rep = lax.axis_index("rep")
        low, high = rep % 2, rep // 2
        to_low, to_high = rep + 1 - 2 * low, rep + 2 - 4 * high
        self.near, self.far = (to_high, to_low) if swap else (to_low, to_high)
        mine, other = (high, low) if swap else (low, high)
        self.half, self.part = rows // 2, rows // 4
        self.mine, self.other = mine, other
        self.keep = row + mine * self.half
        self.give = row + (1 - mine) * self.half

    def copy(self, which, source, target, rep):
        return pltpu.make_async_remote_copy(
            source,
            target,
            self.sems.at[0, self.at, which],
            self.sems.at[1, self.at, which],
            device_id={"rep": rep},
            device_id_type=MESH,
        )

    def rows(self, start, count):
        return pl.ds(pl.multiple_of(start, self.part), count)

    def place(self, flip):
        part = self.keep + (1 - self.other if flip else self.other) * self.part
        return self.out.at[self.rows(part, self.part), self.cols]

    def hop(self, which):
        cols = self.cols
        if which == 0:
            return self.copy(0, self.stage.at[:, cols], self.first.at[:, cols], self.near)
        if which == 1:
            return self.copy(1, self.second.at[0, :, cols], self.second.at[1, :, cols], self.far)
        if which == 4:
            return self.copy(4, self.place(True), self.place(True), self.near)
        to = self.far if which == 2 else self.near
        return self.copy(which, self.done.at[:, cols], self.place(False), to)

    def local(self):
        done = self.done.at[:, self.cols]
        return pltpu.make_async_copy(done, self.place(False), self.sems.at[0, self.at, 5])

    def start(self):
        self.stage[:, self.cols] = self.acc[self.rows(self.give, self.half), self.cols].astype(BF16)
        self.hop(0).start()

    def middle(self):
        part, cols = self.part, self.cols
        self.hop(0).wait_recv()
        other = self.first[self.rows((1 - self.other) * part, part), cols].astype(F32)
        given = self.acc[self.rows(self.keep + (1 - self.other) * part, part), cols] + other
        self.second[0, :, cols] = given.astype(BF16)
        self.hop(1).start()

    def finish(self):
        part, cols = self.part, self.cols
        self.hop(1).wait_recv()
        total = self.acc[self.rows(self.keep + self.other * part, part), cols]
        total = total + self.first[self.rows(self.other * part, part), cols].astype(F32)
        total = total + self.second[1, :, cols].astype(F32)
        self.done[:, cols] = total.astype(BF16)
        self.hop(2).start()
        self.hop(3).start()
        self.local().start()

    def forward(self):
        self.hop(2).wait_recv()
        self.hop(4).start()

    def drain(self):
        self.hop(3).wait_recv()
        self.hop(4).wait_recv()
        for which in range(5):
            self.hop(which).wait_send()
        self.local().wait()


def kernel(
    sizes,
    inputs_hbm,
    cot_hbm,
    gate_hbm,
    up_hbm,
    gate_w_hbm,
    up_w_hbm,
    down_w_hbm,
    input_out,
    gate_out,
    up_out,
    down_out,
    cot,
    down_w,
    inputs,
    gate_w,
    up_w,
    gate_acc,
    up_acc,
    down_acc,
    gate_buf,
    up_buf,
    gate_delta,
    up_delta,
    partial,
    partial_in,
    input_fin,
    gate_stage,
    gate_first,
    gate_second,
    gate_done,
    up_stage,
    up_first,
    up_second,
    up_done,
    down_stage,
    down_first,
    down_second,
    down_done,
    load_sem,
    buf_sem,
    line_recv,
    line_right,
    line_left,
    pair_send,
    pair_recv,
    own_sem,
    weight_recv,
    weight_send,
    peer_sem,
    part_send,
    part_recv,
    sum_sem,
    out_sem,
):
    tps, slabs, side, width, hidden, block, scale = sizes
    tokens = 2 * side
    rep, fs, tp = lax.axis_index("rep"), lax.axis_index("fs"), lax.axis_index("tp")
    pair = 1 - fs
    low, high = rep % 2, rep // 2
    peers = [rep + 1 - 2 * low, rep + 2 - 4 * high, 3 - rep]
    quarter = hidden // 4

    barrier = pltpu.get_barrier_semaphore()

    def greet(where):
        pl.semaphore_signal(barrier, 1, device_id=where, device_id_type=MESH)

    greet({"fs": pair})
    for peer in peers:
        greet({"rep": peer})

    @pl.when(tp > 0)
    def _():
        greet({"tp": tp - 1})

    @pl.when(tp < tps - 1)
    def _():
        greet({"tp": tp + 1})

    neighbours = jnp.minimum(tp, 1) + jnp.minimum(tps - 1 - tp, 1)
    pl.semaphore_wait(barrier, 4 + neighbours)

    def lanes(origin):
        return pl.ds(pl.multiple_of(origin * width, width), width)

    def remote(source, target, send, recv, where):
        return pltpu.make_async_remote_copy(
            source, target, send, recv, device_id=where, device_id_type=MESH
        )

    def weight_slot(origin, group):
        rows = pl.ds(pl.multiple_of(group * quarter, quarter), quarter)
        return down_w.at[rows, lanes(origin)]

    def weight_line(origin, to, side_at, own):
        rows = pl.ds(pl.multiple_of(rep * quarter, quarter), quarter)
        source = down_w_hbm.at[rows] if own else weight_slot(origin, rep)
        return remote(
            source,
            weight_slot(origin, rep),
            weight_send.at[side_at, origin],
            weight_recv.at[origin],
            {"tp": to},
        )

    def weight_peer(origin, at):
        slot = weight_slot(origin, rep)
        return remote(
            slot, slot, peer_sem.at[0, origin, at], peer_sem.at[1, origin, at], {"rep": peers[at]}
        )

    def weight_own():
        @pl.when(tp < tps - 1)
        def _():
            weight_line(tp, tp + 1, 0, True).start()

        @pl.when(tp > 0)
        def _():
            weight_line(tp, tp - 1, 1, True).start()

    def weight_step(k):
        origin = tp - k

        @pl.when(origin >= 0)
        def _():
            weight_line(origin, tp, 0, False).wait_recv()

            @pl.when(tp < tps - 1)
            def _():
                weight_line(origin, tp + 1, 0, False).start()

            for at in range(3):
                weight_peer(origin, at).start()

        back = tp + k

        @pl.when(back < tps)
        def _():
            weight_line(back, tp, 1, False).wait_recv()

            @pl.when(tp > 0)
            def _():
                weight_line(back, tp - 1, 1, False).start()

            for at in range(3):
                weight_peer(back, at).start()

    def slot(origin, slab):
        return cot.at[slab, fs, :, lanes(origin)]

    def line(origin, slab, to, sems, own=False):
        source = cot_hbm.at[slab] if own else slot(origin, slab)
        return remote(
            source, slot(origin, slab), sems.at[origin, slab], line_recv.at[origin, slab], {"tp": to}
        )

    def across(origin, slab):
        place = slot(origin, slab)
        return remote(
            place, place, pair_send.at[origin, slab], pair_recv.at[origin, slab], {"fs": pair}
        )

    def send_own(slab):
        @pl.when(tp < tps - 1)
        def _():
            line(tp, slab, tp + 1, line_right, True).start()

        @pl.when(tp > 0)
        def _():
            line(tp, slab, tp - 1, line_left, True).start()

    def forward(step):
        for k in range(1, tps):
            slab = step - k + 1
            inside = jnp.logical_and(slab >= 0, slab < slabs)
            origin = tp - k

            @pl.when(jnp.logical_and(inside, origin >= 0))
            def _():
                line(origin, slab, tp, line_right).wait_recv()

                @pl.when(tp < tps - 1)
                def _():
                    line(origin, slab, tp + 1, line_right).start()

                across(origin, slab).start()

            back = tp + k

            @pl.when(jnp.logical_and(inside, back < tps))
            def _():
                line(back, slab, tp, line_left).wait_recv()

                @pl.when(tp > 0)
                def _():
                    line(back, slab, tp - 1, line_left).start()

                across(back, slab).start()

        @pl.when(step + 1 < slabs)
        def _():
            send_own(step + 1)

    weight_own()
    own_cot = remote(cot_hbm, cot.at[:, fs, :, lanes(tp)], own_sem.at[0], own_sem.at[1], {"fs": pair})
    own_cot.start()
    own_inputs = remote(inputs_hbm, inputs.at[:, fs], own_sem.at[2], own_sem.at[3], {"fs": pair})
    own_inputs.start()

    loads = [
        pltpu.make_async_copy(cot_hbm, cot.at[:, fs, :, lanes(tp)], load_sem.at[0]),
        pltpu.make_async_copy(inputs_hbm, inputs.at[:, fs], load_sem.at[1]),
        pltpu.make_async_copy(down_w_hbm, down_w.at[:, lanes(tp)], load_sem.at[2]),
        pltpu.make_async_copy(gate_w_hbm, gate_w, load_sem.at[3]),
        pltpu.make_async_copy(up_w_hbm, up_w, load_sem.at[4]),
    ]

    def fetch(slab):
        return [
            pltpu.make_async_copy(gate_hbm.at[:, slab], gate_buf.at[slab % 2], buf_sem.at[0, slab % 2]),
            pltpu.make_async_copy(up_hbm.at[:, slab], up_buf.at[slab % 2], buf_sem.at[1, slab % 2]),
        ]

    for copy in fetch(0):
        copy.start()
    for copy in loads:
        copy.start()
    send_own(0)

    def arrive(slab, following):
        for copy in fetch(slab):
            copy.wait()

        @pl.when(following < slabs)
        def _():
            for copy in fetch(following):
                copy.start()

    def saved(slab, cols):
        shape = (tokens, block)
        gate = gate_buf[slab % 2, :, :, cols].reshape(shape).astype(F32)
        up = up_buf[slab % 2, :, :, cols].reshape(shape).astype(F32)
        return gate, up, jax.nn.sigmoid(gate)

    def blocks(body):
        def one(at, carry):
            body(pl.ds(pl.multiple_of(at * block, block), block))
            return carry

        lax.fori_loop(0, hidden // block, one, 0)

    gate_acc[...] = jnp.zeros_like(gate_acc)
    up_acc[...] = jnp.zeros_like(up_acc)
    down_acc[...] = jnp.zeros_like(down_acc)
    loads[0].wait()
    own_cot.wait_recv()

    def down_slab(slab, carry):
        arrive(slab, slab + 1)

        def body(cols):
            gate, up, sig = saved(slab, cols)
            act = (gate * sig * up).astype(BF16)
            here = cot[slab, :, :, lanes(tp)].reshape(tokens, width)
            down_acc[cols, :] += dot(act, here, 0, 0) * scale

        blocks(body)
        return carry

    first_part = max(1, (slabs * 6) // 10)
    lax.fori_loop(0, first_part, down_slab, 0)
    weight_step(1)
    lax.fori_loop(first_part, slabs, down_slab, 0)
    for copy in fetch(0):
        copy.start()

    rest = hidden // 2
    sums_down = [
        Sum(
            down_acc,
            down_out,
            at * rest,
            rest,
            pl.ds(0, width),
            at == 1,
            down_stage.at[at],
            down_first.at[at],
            down_second.at[at],
            down_done.at[at],
            sum_sem,
            at,
        )
        for at in range(2)
    ]
    for k in range(2, tps):
        weight_step(k)
    for one in sums_down:
        one.start()

    for copy in loads[1:]:
        copy.wait()
    own_inputs.wait_recv()

    lax.fori_loop(0, tps - 2, lambda i, c: (forward(i), c)[1], 0)
    for one in sums_down:
        one.middle()

    for origin in range(tps):

        @pl.when(tp != origin)
        def _():
            for at in range(3):
                place = weight_slot(origin, peers[at])
                remote(
                    place, place, peer_sem.at[0, origin, at], peer_sem.at[1, origin, at], {"rep": rep}
                ).wait_recv()

    def input_part(slab):
        part = dot(gate_delta[...], gate_w[...], 1, 1) + dot(up_delta[...], up_w[...], 1, 1)
        partial[slab] = part.astype(BF16).reshape(2, side, width)
        give(slab).start()

    def give(slab):
        return remote(
            partial.at[slab, pair],
            partial_in.at[slab],
            part_send.at[slab],
            part_recv.at[slab],
            {"fs": pair},
        )

    def input_sum(slab):
        give(slab).wait_recv()
        total = partial[slab, fs].astype(F32) + partial_in[slab].astype(F32)
        input_fin[slab] = total.astype(BF16)

    def main_slab(slab, carry):
        forward(slab + tps - 2)
        for origin in range(tps):

            @pl.when(tp != origin)
            def _():
                place = cot.at[slab, pair, :, lanes(origin)]
                remote(
                    place,
                    place,
                    pair_send.at[origin, slab],
                    pair_recv.at[origin, slab],
                    {"fs": pair},
                ).wait_recv()

        arrive(slab, slab + 1)
        rows_in = inputs[slab].reshape(tokens, width)

        def body(cols):
            grad = dot(cot[slab].reshape(tokens, tps * width), down_w[cols, :], 1, 1)
            gate, up, sig = saved(slab, cols)
            gate_d = (grad * up * sig * (1.0 + gate * (1.0 - sig))).astype(BF16)
            up_d = (grad * (gate * sig)).astype(BF16)
            gate_delta[:, cols] = gate_d
            up_delta[:, cols] = up_d
            gate_acc[:, cols] += dot(rows_in, gate_d, 0, 0) * scale
            up_acc[:, cols] += dot(rows_in, up_d, 0, 0) * scale

        blocks(body)

        @pl.when(slab < slabs - 1)
        def _():
            input_part(slab)

        @pl.when(slab > 0)
        def _():
            input_sum(slab - 1)

        @pl.when(slab == 1)
        def _():
            for one in sums_down:
                one.finish()

        @pl.when(slab == 3)
        def _():
            for one in sums_down:
                one.forward()

        return carry

    lax.fori_loop(0, slabs, main_slab, 0)

    chunk = hidden // 3
    sums = []
    for at in range(3):
        cols = pl.ds(at * chunk, chunk)
        sums.append(
            Sum(gate_acc, gate_out, 0, width, cols, False, gate_stage, gate_first, gate_second,
                gate_done, sum_sem, 2 + 2 * at)
        )
        sums.append(
            Sum(up_acc, up_out, 0, width, cols, True, up_stage, up_first, up_second, up_done,
                sum_sem, 3 + 2 * at)
        )
    for one in sums:
        one.start()
    input_part(slabs - 1)
    for one in sums:
        one.middle()
    input_sum(slabs - 1)
    out_copy = pltpu.make_async_copy(input_fin, input_out, out_sem.at[0])
    out_copy.start()
    for one in sums:
        one.finish()
    for one in sums:
        one.forward()

    own_cot.wait_send()
    own_inputs.wait_send()
    out_copy.wait()

    def drain_slab(slab, carry):
        give(slab).wait_send()
        for origin in range(tps):
            sent_right = jnp.logical_and(origin <= tp, tp < tps - 1)
            sent_left = jnp.logical_and(origin >= tp, tp > 0)

            @pl.when(sent_right)
            def _():
                line(origin, slab, tp, line_right).wait_send()

            @pl.when(sent_left)
            def _():
                line(origin, slab, tp, line_left).wait_send()

            @pl.when(tp != origin)
            def _():
                across(origin, slab).wait_send()

        return carry

    lax.fori_loop(0, slabs, drain_slab, 0)
    for origin in range(tps):

        @pl.when(jnp.logical_and(origin <= tp, tp < tps - 1))
        def _():
            weight_line(origin, tp, 0, False).wait_send()

        @pl.when(jnp.logical_and(origin >= tp, tp > 0))
        def _():
            weight_line(origin, tp, 1, False).wait_send()

        @pl.when(tp != origin)
        def _():
            for at in range(3):
                weight_peer(origin, at).wait_send()

    for one in sums_down + sums:
        one.drain()


def on_device(layer_input, cotangent, gate_pre, up_pre, gate_weight, up_weight, down_weight):
    tps, groups = lax.axis_size("tp"), lax.axis_size("rep")
    rows, width = layer_input.shape
    hidden = gate_pre.shape[1]
    side = math.gcd(rows, 128)
    slabs = rows // side
    block = math.gcd(hidden, 512)
    scale = 1.0 / math.sqrt(rows * groups * lax.axis_size("fs"))
    sizes = (tps, slabs, side, width, hidden, block, scale)
    half, part = width // 2, width // 4
    rest = hidden // 2
    vmem = pltpu.VMEM
    dma = pltpu.SemaphoreType.DMA
    anywhere = pl.BlockSpec(memory_space=pl.ANY)
    pieces = lambda value: value.reshape(slabs, side, value.shape[1])
    both = lambda value: value.reshape(2, slabs, side, value.shape[1])
    sums_of = lambda n: [
        vmem((half, hidden), BF16),
        vmem((half, hidden), BF16),
        vmem((2, part, hidden), BF16),
        vmem((part, hidden), BF16),
    ]
    tokens = 2 * side
    input_grad, gate_grad, up_grad, down_grad = pl.pallas_call(
        functools.partial(kernel, sizes),
        out_shape=(
            jax.ShapeDtypeStruct((slabs, side, width), BF16),
            jax.ShapeDtypeStruct((width, hidden), BF16),
            jax.ShapeDtypeStruct((width, hidden), BF16),
            jax.ShapeDtypeStruct((hidden, width), BF16),
        ),
        in_specs=[anywhere] * 7,
        out_specs=(anywhere,) * 4,
        scratch_shapes=[
            vmem((slabs, 2, side, tps * width), BF16),
            vmem((hidden, tps * width), BF16),
            vmem((slabs, 2, side, width), BF16),
            vmem((width, hidden), BF16),
            vmem((width, hidden), BF16),
            vmem((width, hidden), F32),
            vmem((width, hidden), F32),
            vmem((hidden, width), F32),
            vmem((2, 2, side, hidden), BF16),
            vmem((2, 2, side, hidden), BF16),
            vmem((tokens, hidden), BF16),
            vmem((tokens, hidden), BF16),
            vmem((slabs, 2, side, width), BF16),
            vmem((slabs, side, width), BF16),
            vmem((slabs, side, width), BF16),
        ]
        + sums_of(0)
        + sums_of(1)
        + [
            vmem((2, rest // 2, width), BF16),
            vmem((2, rest // 2, width), BF16),
            vmem((2, 2, rest // 4, width), BF16),
            vmem((2, rest // 4, width), BF16),
            dma((5,)),
            dma((2, 2)),
            dma((tps, slabs)),
            dma((tps, slabs)),
            dma((tps, slabs)),
            dma((tps, slabs)),
            dma((tps, slabs)),
            dma((4,)),
            dma((tps,)),
            dma((2, tps)),
            dma((2, tps, 3)),
            dma((slabs,)),
            dma((slabs,)),
            dma((2, 8, 6)),
            dma((1,)),
        ],
        compiler_params=pltpu.CompilerParams(
            collective_id=0, has_side_effects=True, vmem_limit_bytes=62 * 2**20
        ),
        name="backward",
    )(
        pieces(layer_input),
        pieces(cotangent),
        both(gate_pre),
        both(up_pre),
        gate_weight,
        up_weight,
        down_weight,
    )
    input_grad = input_grad.reshape(rows, width)
    gate_grad, up_grad, down_grad = (v.astype(F32) for v in (gate_grad, up_grad, down_grad))
    gate_sq = jnp.sum(gate_grad * gate_grad, axis=1)
    up_sq = jnp.sum(up_grad * up_grad, axis=1)
    squares = sum_small(jnp.stack([gate_sq, up_sq]), "fs")
    down_sq = sum_small(jnp.sum(down_grad * down_grad, axis=1), "tp")
    return (input_grad, gate_grad, up_grad, down_grad, squares[0], squares[1], down_sq)


def solution(mesh):
    return jax.shard_map(
        on_device,
        mesh=mesh,
        in_specs=(
            P(("rep", "fs"), "tp"),
            P(("rep", "fs"), "tp"),
            P("rep", "fs"),
            P("rep", "fs"),
            P("tp", "fs"),
            P("tp", "fs"),
            P("fs", "tp"),
        ),
        out_specs=(
            P(("rep", "fs"), "tp"),
            P("tp", "fs"),
            P("tp", "fs"),
            P("fs", "tp"),
            P("tp"),
            P("tp"),
            P("fs"),
        ),
        check_vma=False,
    )
```

```python
import functools
import math

import jax
import jax.numpy as jnp
from jax import lax
from jax.experimental import pallas as pl
from jax.experimental.pallas import tpu as pltpu
from jax.sharding import PartitionSpec as P

MESH = pl.DeviceIdType.MESH
F32 = jnp.float32
BF16 = jnp.bfloat16


def dot(left_side, right_side, left_dim, right_dim):
    return lax.dot_general(
        left_side,
        right_side,
        (((left_dim,), (right_dim,)), ((), ())),
        preferred_element_type=F32,
    )


def fold(values):
    values = values.astype(F32)
    squares = values * values
    return sum(squares[:, at : at + 128] for at in range(0, values.shape[1], 128))


def row_sums(folded):
    return jnp.sum(folded.T, axis=0, keepdims=True)


class Sum:
    def __init__(self, acc, out, row, rows, cols, swap, stage, first, second, full, sems, at):
        self.acc, self.out, self.cols, self.sems, self.at = acc, out, cols, sems, at
        self.stage, self.first, self.second, self.full = stage, first, second, full
        self.all = pl.ds(row, rows)
        rep = lax.axis_index("rep")
        low, high = rep % 2, rep // 2
        to_low, to_high = rep + 1 - 2 * low, rep + 2 - 4 * high
        self.near, self.far = (to_high, to_low) if swap else (to_low, to_high)
        mine, other = (high, low) if swap else (low, high)
        self.half, self.part = rows // 2, rows // 4
        self.mine, self.other = mine, other
        self.keep = row + mine * self.half
        self.give = row + (1 - mine) * self.half

    def copy(self, which, source, target, rep):
        return pltpu.make_async_remote_copy(
            source,
            target,
            self.sems.at[0, self.at, which],
            self.sems.at[1, self.at, which],
            device_id={"rep": rep},
            device_id_type=MESH,
        )

    def rows(self, start, count):
        return pl.ds(pl.multiple_of(start, self.part), count)

    def place(self, flip):
        part = self.keep + (1 - self.other if flip else self.other) * self.part
        return self.full.at[self.rows(part, self.part), self.cols]

    def hop(self, which):
        cols = self.cols
        if which == 0:
            return self.copy(0, self.stage.at[:, cols], self.first.at[:, cols], self.near)
        if which == 1:
            return self.copy(1, self.second.at[0, :, cols], self.second.at[1, :, cols], self.far)
        if which == 4:
            return self.copy(4, self.place(True), self.place(True), self.near)
        to = self.far if which == 2 else self.near
        return self.copy(which, self.place(False), self.place(False), to)

    def local(self):
        here = (self.all, self.cols)
        return pltpu.make_async_copy(
            self.full.at[here], self.out.at[here], self.sems.at[0, self.at, 5]
        )

    def start(self):
        self.stage[:, self.cols] = self.acc[self.rows(self.give, self.half), self.cols].astype(BF16)
        self.hop(0).start()

    def middle(self):
        part, cols = self.part, self.cols
        self.hop(0).wait_recv()
        other = self.first[self.rows((1 - self.other) * part, part), cols].astype(F32)
        given = self.acc[self.rows(self.keep + (1 - self.other) * part, part), cols] + other
        self.second[0, :, cols] = given.astype(BF16)
        self.hop(1).start()

    def finish(self):
        part, cols = self.part, self.cols
        self.hop(1).wait_recv()
        total = self.acc[self.rows(self.keep + self.other * part, part), cols]
        total = total + self.first[self.rows(self.other * part, part), cols].astype(F32)
        total = total + self.second[1, :, cols].astype(F32)
        self.full[self.rows(self.keep + self.other * part, part), cols] = total.astype(BF16)
        self.hop(2).start()
        self.hop(3).start()

    def forward(self):
        self.hop(2).wait_recv()
        self.hop(4).start()

    def collect(self):
        self.hop(3).wait_recv()
        self.hop(4).wait_recv()
        self.local().start()

    def drain(self):
        for which in range(5):
            self.hop(which).wait_send()
        self.local().wait()


def kernel(
    sizes,
    inputs_hbm,
    cot_hbm,
    gate_hbm,
    up_hbm,
    gate_w_hbm,
    up_w_hbm,
    down_w_hbm,
    input_out,
    gate_out,
    up_out,
    down_out,
    rows_out,
    down_rows_out,
    cot,
    down_w,
    inputs,
    gate_w,
    up_w,
    gate_acc,
    up_acc,
    down_acc,
    gate_buf,
    up_buf,
    gate_delta,
    up_delta,
    partial,
    partial_in,
    input_fin,
    gate_stage,
    gate_first,
    gate_second,
    gate_full,
    up_stage,
    up_first,
    up_second,
    up_full,
    down_stage,
    down_first,
    down_second,
    down_full,
    folded,
    squares,
    down_squares,
    load_sem,
    buf_sem,
    line_recv,
    line_right,
    line_left,
    pair_send,
    pair_recv,
    own_sem,
    weight_recv,
    weight_send,
    peer_sem,
    part_send,
    part_recv,
    sum_sem,
    out_sem,
    square_sem,
    down_square_sem,
):
    tps, slabs, side, width, hidden, block, ahead, scale = sizes
    tokens = 2 * side
    rep, fs, tp = lax.axis_index("rep"), lax.axis_index("fs"), lax.axis_index("tp")
    pair = 1 - fs
    low, high = rep % 2, rep // 2
    peers = [rep + 1 - 2 * low, rep + 2 - 4 * high, 3 - rep]
    quarter, half = hidden // 4, hidden // 8

    barrier = pltpu.get_barrier_semaphore()

    def greet(where):
        pl.semaphore_signal(barrier, 1, device_id=where, device_id_type=MESH)

    greet({"fs": pair})
    for peer in peers:
        greet({"rep": peer})

    for by in range(1, tps):
        greet({"tp": (tp + by) % tps})
    pl.semaphore_wait(barrier, 3 + tps)

    def lanes(origin):
        return pl.ds(pl.multiple_of(origin * width, width), width)

    def remote(source, target, send, recv, where):
        return pltpu.make_async_remote_copy(
            source, target, send, recv, device_id=where, device_id_type=MESH
        )

    def weight_slot(origin, group):
        rows = pl.ds(pl.multiple_of(group * quarter, quarter), quarter)
        return down_w.at[rows, lanes(origin)]

    def weight_line(origin, to, side_at, own):
        rows = pl.ds(pl.multiple_of(rep * quarter, quarter), quarter)
        source = down_w_hbm.at[rows] if own else weight_slot(origin, rep)
        return remote(
            source,
            weight_slot(origin, rep),
            weight_send.at[side_at, origin],
            weight_recv.at[origin],
            {"tp": to},
        )

    def weight_half(origin, group, late):
        rows = pl.ds(pl.multiple_of(group * quarter + late * half, half), half)
        return down_w.at[rows, lanes(origin)]

    def weight_peer(origin, at):
        if at < 2:
            place = weight_slot(origin, rep)
        else:
            place = weight_half(origin, peers[at - 2], at - 2)
        to = peers[at % 2 if at < 2 else 3 - at]
        return remote(
            place, place, peer_sem.at[0, origin, at], peer_sem.at[1, origin, at], {"rep": to}
        )

    def weight_from(origin, at):
        if at < 2:
            place = weight_slot(origin, peers[at])
        else:
            place = weight_half(origin, peers[2], at - 2)
        return remote(
            place, place, peer_sem.at[0, origin, at], peer_sem.at[1, origin, at], {"rep": peers[0]}
        )

    def weight_relay(k):
        for origin, inside in ((tp - k, tp >= k), (tp + k, tp + k < tps)):

            @pl.when(inside)
            def _():
                for at in range(2):
                    weight_from(origin, at).wait_recv()
                    weight_peer(origin, at + 2).start()

    def weight_own():
        @pl.when(tp < tps - 1)
        def _():
            weight_line(tp, tp + 1, 0, True).start()

        @pl.when(tp > 0)
        def _():
            weight_line(tp, tp - 1, 1, True).start()

    def weight_step(k):
        origin = tp - k

        @pl.when(origin >= 0)
        def _():
            weight_line(origin, tp, 0, False).wait_recv()

            @pl.when(tp < tps - 1)
            def _():
                weight_line(origin, tp + 1, 0, False).start()

            for at in range(2):
                weight_peer(origin, at).start()

        back = tp + k

        @pl.when(back < tps)
        def _():
            weight_line(back, tp, 1, False).wait_recv()

            @pl.when(tp > 0)
            def _():
                weight_line(back, tp - 1, 1, False).start()

            for at in range(2):
                weight_peer(back, at).start()

    def slot(origin, slab):
        return cot.at[slab, fs, :, lanes(origin)]

    def line(origin, slab, to, sems, own=False):
        source = cot_hbm.at[slab] if own else slot(origin, slab)
        return remote(
            source, slot(origin, slab), sems.at[origin], line_recv.at[origin, slab], {"tp": to}
        )

    def across(origin, slab):
        place = slot(origin, slab)
        return remote(
            place, place, pair_send.at[origin], pair_recv.at[origin, slab], {"fs": pair}
        )

    def send_own(slab):
        @pl.when(tp < tps - 1)
        def _():
            line(tp, slab, tp + 1, line_right, True).start()

        @pl.when(tp > 0)
        def _():
            line(tp, slab, tp - 1, line_left, True).start()

    def forward(step):
        for k in range(1, tps):
            slab = step - k + 1
            inside = jnp.logical_and(slab >= 0, slab < slabs)
            origin = tp - k

            @pl.when(jnp.logical_and(inside, origin >= 0))
            def _():
                line(origin, slab, tp, line_right).wait_recv()

                @pl.when(tp < tps - 1)
                def _():
                    line(origin, slab, tp + 1, line_right).start()

                across(origin, slab).start()

            back = tp + k

            @pl.when(jnp.logical_and(inside, back < tps))
            def _():
                line(back, slab, tp, line_left).wait_recv()

                @pl.when(tp > 0)
                def _():
                    line(back, slab, tp - 1, line_left).start()

                across(back, slab).start()

        @pl.when(step + 2 < slabs)
        def _():
            send_own(step + 2)

    weight_own()
    own_cot = remote(cot_hbm, cot.at[:, fs, :, lanes(tp)], own_sem.at[0], own_sem.at[1], {"fs": pair})
    own_cot.start()
    own_inputs = remote(inputs_hbm, inputs.at[:, fs], own_sem.at[2], own_sem.at[3], {"fs": pair})
    own_inputs.start()

    loads = [
        pltpu.make_async_copy(cot_hbm, cot.at[:, fs, :, lanes(tp)], load_sem.at[0]),
        pltpu.make_async_copy(inputs_hbm, inputs.at[:, fs], load_sem.at[1]),
        pltpu.make_async_copy(down_w_hbm, down_w.at[:, lanes(tp)], load_sem.at[2]),
        pltpu.make_async_copy(gate_w_hbm, gate_w, load_sem.at[3]),
        pltpu.make_async_copy(up_w_hbm, up_w, load_sem.at[4]),
    ]

    def fetch(slab):
        return [
            pltpu.make_async_copy(gate_hbm.at[:, slab], gate_buf.at[slab % 2], buf_sem.at[0, slab % 2]),
            pltpu.make_async_copy(up_hbm.at[:, slab], up_buf.at[slab % 2], buf_sem.at[1, slab % 2]),
        ]

    for copy in fetch(0):
        copy.start()
    for copy in loads:
        copy.start()
    send_own(0)

    def arrive(slab, following):
        for copy in fetch(slab):
            copy.wait()

        @pl.when(following < slabs)
        def _():
            for copy in fetch(following):
                copy.start()

    def saved(slab, cols):
        shape = (tokens, block)
        gate = gate_buf[slab % 2, :, :, cols].reshape(shape).astype(F32)
        up = up_buf[slab % 2, :, :, cols].reshape(shape).astype(F32)
        return gate, up, jax.nn.sigmoid(gate)

    def blocks(body):
        def one(at, carry):
            body(pl.ds(pl.multiple_of(at * block, block), block), at)
            return carry

        lax.fori_loop(0, hidden // block, one, 0)

    gate_acc[...] = jnp.zeros_like(gate_acc)
    up_acc[...] = jnp.zeros_like(up_acc)
    down_acc[...] = jnp.zeros_like(down_acc)
    loads[0].wait()
    own_cot.wait_recv()

    def down_slab(slab, carry):
        arrive(slab, slab + 1)

        def body(cols, at):
            gate, up, sig = saved(slab, cols)
            act = (gate * sig * up).astype(BF16)
            here = cot[slab, :, :, lanes(tp)].reshape(tokens, width)
            down_acc[cols, :] += dot(act, here, 0, 0) * scale

        blocks(body)
        return carry

    first_part = max(1, (slabs * 6) // 10)
    lax.fori_loop(0, first_part, down_slab, 0)
    weight_step(1)
    send_own(1)
    lax.fori_loop(first_part, slabs, down_slab, 0)
    for copy in fetch(0):
        copy.start()

    rest = hidden // 2
    sums_down = [
        Sum(
            down_acc,
            down_out,
            at * rest,
            rest,
            pl.ds(0, width),
            at == 1,
            down_stage.at[at],
            down_first.at[at],
            down_second.at[at],
            down_full,
            sum_sem,
            at,
        )
        for at in range(2)
    ]
    for copy in loads[1:]:
        copy.wait()
    for k in range(2, tps):
        weight_step(k)
        forward(k - 2)
        weight_relay(k - 1)
    weight_relay(tps - 1)
    for one in sums_down:
        one.start()
    own_inputs.wait_recv()
    for step in range(tps - 2, tps - 2 + ahead):
        forward(step)

    for origin in range(tps):

        @pl.when(tp != origin)
        def _():
            for at in range(2, 4):
                weight_from(origin, at).wait_recv()

    def input_part(slab):
        part = dot(gate_delta[...], gate_w[...], 1, 1) + dot(up_delta[...], up_w[...], 1, 1)
        partial[slab] = part.astype(BF16).reshape(2, side, width)
        give(slab).start()

    def give(slab):
        return remote(
            partial.at[slab, pair],
            partial_in.at[slab],
            part_send.at[0],
            part_recv.at[slab],
            {"fs": pair},
        )

    def input_sum(slab):
        give(slab).wait_recv()
        total = partial[slab, fs].astype(F32) + partial_in[slab].astype(F32)
        input_fin[slab] = total.astype(BF16)

    def share(by):
        return remote(
            down_squares.at[tp],
            down_squares.at[tp],
            down_square_sem.at[0, by],
            down_square_sem.at[1, by],
            {"tp": (tp + by) % tps},
        )

    def shared(by):
        origin = (tp + tps - by) % tps
        return remote(
            down_squares.at[origin],
            down_squares.at[origin],
            down_square_sem.at[0, by],
            down_square_sem.at[1, by],
            {"tp": origin},
        )

    def pair_sums(at):
        cols = pl.ds(pl.multiple_of(at * block, block), block)
        refs = [
            (gate_acc, gate_out, False, gate_stage, gate_first, gate_second, gate_full),
            (up_acc, up_out, True, up_stage, up_first, up_second, up_full),
        ]
        return [
            Sum(acc, out, 0, width, cols, swap, *rest, sum_sem, 2 + 2 * at + which)
            for which, (acc, out, swap, *rest) in enumerate(refs)
        ]

    late = slabs - 3

    def main_slab(slab, carry):
        lead = jnp.minimum(jnp.maximum(late - slab, 0), 1) * ahead

        @pl.when(slab != late)
        def _():
            forward(slab + tps - 2 + lead)

        for origin in range(tps):

            @pl.when(tp != origin)
            def _():
                place = cot.at[slab, pair, :, lanes(origin)]
                remote(
                    place,
                    place,
                    pair_send.at[origin],
                    pair_recv.at[origin, slab],
                    {"fs": pair},
                ).wait_recv()

        arrive(slab, slab + 1)
        rows_in = inputs[slab].reshape(tokens, width)

        def body(cols, at):
            grad = dot(cot[slab].reshape(tokens, tps * width), down_w[cols, :], 1, 1)
            gate, up, sig = saved(slab, cols)
            gate_d = (grad * up * sig * (1.0 + gate * (1.0 - sig))).astype(BF16)
            up_d = (grad * (gate * sig)).astype(BF16)
            gate_delta[:, cols] = gate_d
            up_delta[:, cols] = up_d
            gate_acc[:, cols] += dot(rows_in, gate_d, 0, 0) * scale
            up_acc[:, cols] += dot(rows_in, up_d, 0, 0) * scale

            @pl.when(slab == slabs - 1)
            def _():
                for one in pair_sums(at):
                    one.start()

        blocks(body)

        @pl.when(slab < slabs - 1)
        def _():
            input_part(slab)

        @pl.when(slab > 0)
        def _():
            input_sum(slab - 1)

        @pl.when(slab == 1)
        def _():
            for one in sums_down:
                one.middle()

        @pl.when(slab == 2)
        def _():
            for one in sums_down:
                one.finish()

        @pl.when(slab == 4)
        def _():
            for one in sums_down:
                one.forward()

        @pl.when(slab == 6)
        def _():
            for one in sums_down:
                one.collect()
            for at in range(hidden // 128):
                values = fold(down_full[at * 128 : at * 128 + 128, :])
                down_squares[tp, at : at + 1, :] = row_sums(values)
            for by in range(1, tps):
                share(by).start()

        return carry

    lax.fori_loop(0, slabs, main_slab, 0)

    sums = [one for at in range(hidden // block) for one in pair_sums(at)]
    input_part(slabs - 1)
    for one in sums:
        one.middle()
    input_sum(slabs - 1)
    out_copy = pltpu.make_async_copy(input_fin, input_out, out_sem.at[0])
    out_copy.start()
    for one in sums:
        one.finish()
    for by in range(1, tps):
        shared(by).wait_recv()
    down_squares[tps] = sum(down_squares[at] for at in range(tps))
    down_rows_copy = pltpu.make_async_copy(down_squares.at[tps], down_rows_out, out_sem.at[1])
    down_rows_copy.start()
    for by in range(1, tps):
        share(by).wait_send()
    for one in sums:
        one.forward()

    for at in range(hidden // block):
        cols = pl.ds(at * block, block)
        for which, one in enumerate(sums[2 * at : 2 * at + 2]):
            one.collect()
            values = fold(one.full[:, cols])
            folded[which] = values if at == 0 else folded[which] + values
    blocks_in = width // 128
    for which in range(2):
        for at in range(blocks_in):
            row = which * blocks_in + at
            squares[0, row : row + 1, :] = row_sums(folded[which, at * 128 : at * 128 + 128, :])
    swap_squares = remote(
        squares.at[0], squares.at[1], square_sem.at[0], square_sem.at[1], {"fs": pair}
    )
    swap_squares.start()

    own_cot.wait_send()
    own_inputs.wait_send()
    out_copy.wait()

    def sent(origin, sems):
        place = cot.at[:, fs, :, lanes(origin)]
        return remote(place, place, sems.at[origin], own_sem.at[1], {"fs": pair})

    for origin in range(tps):

        @pl.when(jnp.logical_and(origin <= tp, tp < tps - 1))
        def _():
            sent(origin, line_right).wait_send()

        @pl.when(jnp.logical_and(origin >= tp, tp > 0))
        def _():
            sent(origin, line_left).wait_send()

        @pl.when(tp != origin)
        def _():
            sent(origin, pair_send).wait_send()

    remote(partial_in, partial_in, part_send.at[0], own_sem.at[1], {"fs": pair}).wait_send()
    for origin in range(tps):

        @pl.when(jnp.logical_and(origin <= tp, tp < tps - 1))
        def _():
            weight_line(origin, tp, 0, False).wait_send()

        @pl.when(jnp.logical_and(origin >= tp, tp > 0))
        def _():
            weight_line(origin, tp, 1, False).wait_send()

        @pl.when(tp != origin)
        def _():
            for at in range(4):
                weight_peer(origin, at).wait_send()

    for one in sums_down + sums:
        one.drain()
    swap_squares.wait()
    squares[2] = squares[0] + squares[1]
    rows_copy = pltpu.make_async_copy(squares.at[2], rows_out, out_sem.at[2])
    rows_copy.start()
    rows_copy.wait()
    down_rows_copy.wait()


def widen_kernel(*refs):
    half = len(refs) // 2
    for source, target in zip(refs[:half], refs[half:]):
        target[...] = source[...].astype(target.dtype)


def widen(values, kinds, steps):
    specs = [pl.BlockSpec((v.shape[0] // steps, v.shape[1]), lambda i: (i, 0)) for v in values]
    return pl.pallas_call(
        widen_kernel,
        grid=(steps,),
        out_shape=[jax.ShapeDtypeStruct(v.shape, kind) for v, kind in zip(values, kinds)],
        in_specs=specs,
        out_specs=specs,
        compiler_params=pltpu.CompilerParams(vmem_limit_bytes=40 * 2**20),
        name="widen",
    )(*values)


def on_device(layer_input, cotangent, gate_pre, up_pre, gate_weight, up_weight, down_weight):
    tps, groups = lax.axis_size("tp"), lax.axis_size("rep")
    rows, width = layer_input.shape
    hidden = gate_pre.shape[1]
    side = math.gcd(rows, 128)
    slabs = rows // side
    block = math.gcd(hidden, 512)
    scale = 1.0 / math.sqrt(rows * groups * lax.axis_size("fs"))
    sizes = (tps, slabs, side, width, hidden, block, 1, scale)
    half, part = width // 2, width // 4
    rest = hidden // 2
    vmem = pltpu.VMEM
    dma = pltpu.SemaphoreType.DMA
    anywhere = pl.BlockSpec(memory_space=pl.ANY)
    pieces = lambda value: value.reshape(slabs, side, value.shape[1])
    both = lambda value: value.reshape(2, slabs, side, value.shape[1])
    sums_of = lambda n: [
        vmem((half, hidden), BF16),
        vmem((half, hidden), BF16),
        vmem((2, part, hidden), BF16),
        vmem((width, hidden), BF16),
    ]
    tokens = 2 * side
    input_grad, gate_grad, up_grad, down_grad, row_squares, down_squares = pl.pallas_call(
        functools.partial(kernel, sizes),
        out_shape=(
            jax.ShapeDtypeStruct((slabs, side, width), BF16),
            jax.ShapeDtypeStruct((width, hidden), BF16),
            jax.ShapeDtypeStruct((width, hidden), BF16),
            jax.ShapeDtypeStruct((hidden, width), BF16),
            jax.ShapeDtypeStruct((2 * width // 128, 128), F32),
            jax.ShapeDtypeStruct((hidden // 128, 128), F32),
        ),
        in_specs=[anywhere] * 7,
        out_specs=(anywhere,) * 6,
        scratch_shapes=[
            vmem((slabs, 2, side, tps * width), BF16),
            vmem((hidden, tps * width), BF16),
            vmem((slabs, 2, side, width), BF16),
            vmem((width, hidden), BF16),
            vmem((width, hidden), BF16),
            vmem((width, hidden), F32),
            vmem((width, hidden), F32),
            vmem((hidden, width), F32),
            vmem((2, 2, side, hidden), BF16),
            vmem((2, 2, side, hidden), BF16),
            vmem((tokens, hidden), BF16),
            vmem((tokens, hidden), BF16),
            vmem((slabs, 2, side, width), BF16),
            vmem((slabs, side, width), BF16),
            vmem((slabs, side, width), BF16),
        ]
        + sums_of(0)
        + sums_of(1)
        + [
            vmem((2, rest // 2, width), BF16),
            vmem((2, rest // 2, width), BF16),
            vmem((2, 2, rest // 4, width), BF16),
            vmem((hidden, width), BF16),
            vmem((2, width, 128), F32),
            vmem((3, 2 * width // 128, 128), F32),
            vmem((tps + 1, hidden // 128, 128), F32),
            dma((5,)),
            dma((2, 2)),
            dma((tps, slabs)),
            dma((tps,)),
            dma((tps,)),
            dma((tps,)),
            dma((tps, slabs)),
            dma((4,)),
            dma((tps,)),
            dma((2, tps)),
            dma((2, tps, 4)),
            dma((1,)),
            dma((slabs,)),
            dma((2, 2 + 2 * (hidden // block), 6)),
            dma((3,)),
            dma((2,)),
            dma((2, tps)),
        ],
        compiler_params=pltpu.CompilerParams(
            collective_id=0, has_side_effects=True, vmem_limit_bytes=62 * 2**20
        ),
        name="backward",
    )(
        pieces(layer_input),
        pieces(cotangent),
        both(gate_pre),
        both(up_pre),
        gate_weight,
        up_weight,
        down_weight,
    )
    input_grad = input_grad.reshape(rows, width)
    input_grad, gate_grad, up_grad, down_grad = widen(
        [input_grad, gate_grad, up_grad, down_grad], [BF16, F32, F32, F32], 4
    )
    squares = row_squares.reshape(2, width)
    return (
        input_grad,
        gate_grad,
        up_grad,
        down_grad,
        squares[0],
        squares[1],
        down_squares.reshape(hidden),
    )


def solution(mesh):
    return jax.shard_map(
        on_device,
        mesh=mesh,
        in_specs=(
            P(("rep", "fs"), "tp"),
            P(("rep", "fs"), "tp"),
            P("rep", "fs"),
            P("rep", "fs"),
            P("tp", "fs"),
            P("tp", "fs"),
            P("fs", "tp"),
        ),
        out_specs=(
            P(("rep", "fs"), "tp"),
            P("tp", "fs"),
            P("tp", "fs"),
            P("fs", "tp"),
            P("tp"),
            P("tp"),
            P("fs"),
        ),
        check_vma=False,
    )
```

```python
import functools
import math

import jax
import jax.numpy as jnp
from jax import lax
from jax.experimental import pallas as pl
from jax.experimental.pallas import tpu as pltpu
from jax.sharding import PartitionSpec as P

MESH = pl.DeviceIdType.MESH
F32 = jnp.float32
BF16 = jnp.bfloat16


def dot(left_side, right_side, left_dim, right_dim):
    return lax.dot_general(
        left_side,
        right_side,
        (((left_dim,), (right_dim,)), ((), ())),
        preferred_element_type=F32,
    )


def fold(values):
    values = values.astype(F32)
    squares = values * values
    return sum(squares[:, at : at + 128] for at in range(0, values.shape[1], 128))


def row_sums(folded):
    return jnp.sum(folded.T, axis=0, keepdims=True)


class Sum:
    def __init__(self, acc, out, row, rows, cols, swap, stage, first, second, full, sems, at):
        self.acc, self.out, self.cols, self.sems, self.at = acc, out, cols, sems, at
        self.stage, self.first, self.second, self.full = stage, first, second, full
        self.all = pl.ds(row, rows)
        rep = lax.axis_index("rep")
        low, high = rep % 2, rep // 2
        to_low, to_high = rep + 1 - 2 * low, rep + 2 - 4 * high
        self.near, self.far = (to_high, to_low) if swap else (to_low, to_high)
        mine, other = (high, low) if swap else (low, high)
        self.half, self.part = rows // 2, rows // 4
        self.mine, self.other = mine, other
        self.keep = row + mine * self.half
        self.give = row + (1 - mine) * self.half

    def copy(self, which, source, target, rep):
        return pltpu.make_async_remote_copy(
            source,
            target,
            self.sems.at[0, self.at, which],
            self.sems.at[1, self.at, which],
            device_id={"rep": rep},
            device_id_type=MESH,
        )

    def rows(self, start, count):
        return pl.ds(pl.multiple_of(start, self.part), count)

    def place(self, flip):
        part = self.keep + (1 - self.other if flip else self.other) * self.part
        return self.full.at[self.rows(part, self.part), self.cols]

    def hop(self, which):
        cols = self.cols
        if which == 0:
            return self.copy(0, self.stage.at[:, cols], self.first.at[:, cols], self.near)
        if which == 1:
            return self.copy(1, self.second.at[0, :, cols], self.second.at[1, :, cols], self.far)
        if which == 4:
            return self.copy(4, self.place(True), self.place(True), self.near)
        to = self.far if which == 2 else self.near
        return self.copy(which, self.place(False), self.place(False), to)

    def local(self):
        here = (self.all, self.cols)
        return pltpu.make_async_copy(
            self.full.at[here], self.out.at[here], self.sems.at[0, self.at, 5]
        )

    def start(self):
        self.stage[:, self.cols] = self.acc[self.rows(self.give, self.half), self.cols].astype(BF16)
        self.hop(0).start()

    def middle(self):
        part, cols = self.part, self.cols
        self.hop(0).wait_recv()
        other = self.first[self.rows((1 - self.other) * part, part), cols].astype(F32)
        given = self.acc[self.rows(self.keep + (1 - self.other) * part, part), cols] + other
        self.second[0, :, cols] = given.astype(BF16)
        self.hop(1).start()

    def finish(self):
        part, cols = self.part, self.cols
        self.hop(1).wait_recv()
        total = self.acc[self.rows(self.keep + self.other * part, part), cols]
        total = total + self.first[self.rows(self.other * part, part), cols].astype(F32)
        total = total + self.second[1, :, cols].astype(F32)
        self.full[self.rows(self.keep + self.other * part, part), cols] = total.astype(BF16)
        self.hop(2).start()
        self.hop(3).start()

    def forward(self):
        self.hop(2).wait_recv()
        self.hop(4).start()

    def collect(self):
        self.hop(3).wait_recv()
        self.hop(4).wait_recv()
        self.local().start()

    def drain(self):
        for which in range(5):
            self.hop(which).wait_send()
        self.local().wait()


def kernel(
    sizes,
    inputs_hbm,
    cot_hbm,
    gate_hbm,
    up_hbm,
    gate_w_hbm,
    up_w_hbm,
    down_w_hbm,
    input_out,
    gate_out,
    up_out,
    down_out,
    rows_out,
    down_rows_out,
    cot,
    down_w,
    inputs,
    gate_w,
    up_w,
    gate_acc,
    up_acc,
    down_acc,
    gate_buf,
    up_buf,
    gate_delta,
    up_delta,
    partial,
    partial_in,
    input_fin,
    gate_stage,
    gate_first,
    gate_second,
    gate_full,
    up_stage,
    up_first,
    up_second,
    up_full,
    down_stage,
    down_first,
    down_second,
    down_full,
    folded,
    squares,
    down_squares,
    load_sem,
    buf_sem,
    line_recv,
    line_right,
    line_left,
    pair_send,
    pair_recv,
    own_sem,
    weight_recv,
    weight_send,
    peer_sem,
    part_send,
    part_recv,
    sum_sem,
    out_sem,
    square_sem,
    down_square_sem,
):
    tps, slabs, side, width, hidden, block, ahead, scale = sizes
    tokens = 2 * side
    rep, fs, tp = lax.axis_index("rep"), lax.axis_index("fs"), lax.axis_index("tp")
    pair = 1 - fs
    low, high = rep % 2, rep // 2
    peers = [rep + 1 - 2 * low, rep + 2 - 4 * high, 3 - rep]
    quarter, half = hidden // 4, hidden // 8

    barrier = pltpu.get_barrier_semaphore()

    def greet(where):
        pl.semaphore_signal(barrier, 1, device_id=where, device_id_type=MESH)

    greet({"fs": pair})
    for peer in peers:
        greet({"rep": peer})

    for by in range(1, tps):
        greet({"tp": (tp + by) % tps})
    pl.semaphore_wait(barrier, 3 + tps)

    def lanes(origin):
        return pl.ds(pl.multiple_of(origin * width, width), width)

    def remote(source, target, send, recv, where):
        return pltpu.make_async_remote_copy(
            source, target, send, recv, device_id=where, device_id_type=MESH
        )

    def weight_slot(origin, group):
        rows = pl.ds(pl.multiple_of(group * quarter, quarter), quarter)
        return down_w.at[rows, lanes(origin)]

    def weight_line(origin, to, side_at, own):
        rows = pl.ds(pl.multiple_of(rep * quarter, quarter), quarter)
        source = down_w_hbm.at[rows] if own else weight_slot(origin, rep)
        return remote(
            source,
            weight_slot(origin, rep),
            weight_send.at[side_at, origin],
            weight_recv.at[origin],
            {"tp": to},
        )

    def weight_half(origin, group, late):
        rows = pl.ds(pl.multiple_of(group * quarter + late * half, half), half)
        return down_w.at[rows, lanes(origin)]

    def weight_peer(origin, at):
        if at < 2:
            place = weight_slot(origin, rep)
        else:
            place = weight_half(origin, peers[at - 2], at - 2)
        to = peers[at % 2 if at < 2 else 3 - at]
        return remote(
            place, place, peer_sem.at[0, origin, at], peer_sem.at[1, origin, at], {"rep": to}
        )

    def weight_from(origin, at):
        if at < 2:
            place = weight_slot(origin, peers[at])
        else:
            place = weight_half(origin, peers[2], at - 2)
        return remote(
            place, place, peer_sem.at[0, origin, at], peer_sem.at[1, origin, at], {"rep": peers[0]}
        )

    def weight_relay(k):
        for origin, inside in ((tp - k, tp >= k), (tp + k, tp + k < tps)):

            @pl.when(inside)
            def _():
                for at in range(2):
                    weight_from(origin, at).wait_recv()
                    weight_peer(origin, at + 2).start()

    def weight_own():
        @pl.when(tp < tps - 1)
        def _():
            weight_line(tp, tp + 1, 0, True).start()

        @pl.when(tp > 0)
        def _():
            weight_line(tp, tp - 1, 1, True).start()

    def weight_step(k):
        origin = tp - k

        @pl.when(origin >= 0)
        def _():
            weight_line(origin, tp, 0, False).wait_recv()

            @pl.when(tp < tps - 1)
            def _():
                weight_line(origin, tp + 1, 0, False).start()

            for at in range(2):
                weight_peer(origin, at).start()

        back = tp + k

        @pl.when(back < tps)
        def _():
            weight_line(back, tp, 1, False).wait_recv()

            @pl.when(tp > 0)
            def _():
                weight_line(back, tp - 1, 1, False).start()

            for at in range(2):
                weight_peer(back, at).start()

    def slot(origin, slab):
        return cot.at[slab, fs, :, lanes(origin)]

    def line(origin, slab, to, sems, own=False):
        source = cot_hbm.at[slab] if own else slot(origin, slab)
        return remote(
            source, slot(origin, slab), sems.at[origin], line_recv.at[origin, slab], {"tp": to}
        )

    def across(origin, slab):
        place = slot(origin, slab)
        return remote(
            place, place, pair_send.at[origin], pair_recv.at[origin, slab], {"fs": pair}
        )

    def send_own(slab):
        @pl.when(tp < tps - 1)
        def _():
            line(tp, slab, tp + 1, line_right, True).start()

        @pl.when(tp > 0)
        def _():
            line(tp, slab, tp - 1, line_left, True).start()

    def forward(step):
        for k in range(1, tps):
            slab = step - k + 1
            inside = jnp.logical_and(slab >= 0, slab < slabs)
            origin = tp - k

            @pl.when(jnp.logical_and(inside, origin >= 0))
            def _():
                line(origin, slab, tp, line_right).wait_recv()

                @pl.when(tp < tps - 1)
                def _():
                    line(origin, slab, tp + 1, line_right).start()

                across(origin, slab).start()

            back = tp + k

            @pl.when(jnp.logical_and(inside, back < tps))
            def _():
                line(back, slab, tp, line_left).wait_recv()

                @pl.when(tp > 0)
                def _():
                    line(back, slab, tp - 1, line_left).start()

                across(back, slab).start()

        @pl.when(step + 2 < slabs)
        def _():
            send_own(step + 2)

    weight_own()
    own_cot = remote(cot_hbm, cot.at[:, fs, :, lanes(tp)], own_sem.at[0], own_sem.at[1], {"fs": pair})
    own_cot.start()
    own_inputs = remote(inputs_hbm, inputs.at[:, fs], own_sem.at[2], own_sem.at[3], {"fs": pair})
    own_inputs.start()

    loads = [
        pltpu.make_async_copy(cot_hbm, cot.at[:, fs, :, lanes(tp)], load_sem.at[0]),
        pltpu.make_async_copy(inputs_hbm, inputs.at[:, fs], load_sem.at[1]),
        pltpu.make_async_copy(down_w_hbm, down_w.at[:, lanes(tp)], load_sem.at[2]),
        pltpu.make_async_copy(gate_w_hbm, gate_w, load_sem.at[3]),
        pltpu.make_async_copy(up_w_hbm, up_w, load_sem.at[4]),
    ]

    def fetch(slab):
        return [
            pltpu.make_async_copy(gate_hbm.at[:, slab], gate_buf.at[slab % 2], buf_sem.at[0, slab % 2]),
            pltpu.make_async_copy(up_hbm.at[:, slab], up_buf.at[slab % 2], buf_sem.at[1, slab % 2]),
        ]

    for copy in fetch(0):
        copy.start()
    for copy in loads:
        copy.start()
    send_own(0)

    def arrive(slab, following):
        for copy in fetch(slab):
            copy.wait()

        @pl.when(following < slabs)
        def _():
            for copy in fetch(following):
                copy.start()

    def saved(slab, cols):
        shape = (tokens, block)
        gate = gate_buf[slab % 2, :, :, cols].reshape(shape).astype(F32)
        up = up_buf[slab % 2, :, :, cols].reshape(shape).astype(F32)
        return gate, up, jax.nn.sigmoid(gate)

    def blocks(body):
        def one(at, carry):
            body(pl.ds(pl.multiple_of(at * block, block), block), at)
            return carry

        lax.fori_loop(0, hidden // block, one, 0)

    gate_acc[...] = jnp.zeros_like(gate_acc)
    up_acc[...] = jnp.zeros_like(up_acc)
    down_acc[...] = jnp.zeros_like(down_acc)
    loads[0].wait()
    own_cot.wait_recv()

    def down_slab(slab, carry):
        arrive(slab, slab + 1)

        def body(cols, at):
            gate, up, sig = saved(slab, cols)
            act = (gate * sig * up).astype(BF16)
            here = cot[slab, :, :, lanes(tp)].reshape(tokens, width)
            down_acc[cols, :] += dot(act, here, 0, 0) * scale

        blocks(body)
        return carry

    first_part = max(1, (slabs * 6) // 10)
    lax.fori_loop(0, first_part, down_slab, 0)
    weight_step(1)
    send_own(1)
    lax.fori_loop(first_part, slabs, down_slab, 0)
    for copy in fetch(0):
        copy.start()

    rest = hidden // 2
    sums_down = [
        Sum(
            down_acc,
            down_out,
            at * rest,
            rest,
            pl.ds(0, width),
            at == 1,
            down_stage.at[at],
            down_first.at[at],
            down_second.at[at],
            down_full,
            sum_sem,
            at,
        )
        for at in range(2)
    ]
    for copy in loads[1:]:
        copy.wait()
    for k in range(2, tps):
        weight_step(k)
        forward(k - 2)
        weight_relay(k - 1)
    weight_relay(tps - 1)
    for one in sums_down:
        one.start()
    own_inputs.wait_recv()
    for step in range(tps - 2, tps - 2 + ahead):
        forward(step)

    for origin in range(tps):

        @pl.when(tp != origin)
        def _():
            for at in range(2, 4):
                weight_from(origin, at).wait_recv()

    def input_part(slab):
        part = dot(gate_delta[...], gate_w[...], 1, 1) + dot(up_delta[...], up_w[...], 1, 1)
        partial[slab] = part.astype(BF16).reshape(2, side, width)
        give(slab).start()

    def give(slab):
        return remote(
            partial.at[slab, pair],
            partial_in.at[slab],
            part_send.at[0],
            part_recv.at[slab],
            {"fs": pair},
        )

    def input_sum(slab):
        give(slab).wait_recv()
        total = partial[slab, fs].astype(F32) + partial_in[slab].astype(F32)
        input_fin[slab] = total.astype(BF16)

    def share(by):
        return remote(
            down_squares.at[tp],
            down_squares.at[tp],
            down_square_sem.at[0, by],
            down_square_sem.at[1, by],
            {"tp": (tp + by) % tps},
        )

    def shared(by):
        origin = (tp + tps - by) % tps
        return remote(
            down_squares.at[origin],
            down_squares.at[origin],
            down_square_sem.at[0, by],
            down_square_sem.at[1, by],
            {"tp": origin},
        )

    def pair_sums(at):
        cols = pl.ds(pl.multiple_of(at * block, block), block)
        refs = [
            (gate_acc, gate_out, False, gate_stage, gate_first, gate_second, gate_full),
            (up_acc, up_out, True, up_stage, up_first, up_second, up_full),
        ]
        return [
            Sum(acc, out, 0, width, cols, swap, *rest, sum_sem, 2 + 2 * at + which)
            for which, (acc, out, swap, *rest) in enumerate(refs)
        ]

    late = slabs // 2

    def main_slab(slab, carry):
        lead = jnp.minimum(jnp.maximum(late - slab, 0), 1) * ahead

        @pl.when(slab != late)
        def _():
            forward(slab + tps - 2 + lead)

        for origin in range(tps):

            @pl.when(tp != origin)
            def _():
                place = cot.at[slab, pair, :, lanes(origin)]
                remote(
                    place,
                    place,
                    pair_send.at[origin],
                    pair_recv.at[origin, slab],
                    {"fs": pair},
                ).wait_recv()

        arrive(slab, slab + 1)
        rows_in = inputs[slab].reshape(tokens, width)

        def body(cols, at):
            grad = dot(cot[slab].reshape(tokens, tps * width), down_w[cols, :], 1, 1)
            gate, up, sig = saved(slab, cols)
            gate_d = (grad * up * sig * (1.0 + gate * (1.0 - sig))).astype(BF16)
            up_d = (grad * (gate * sig)).astype(BF16)
            gate_delta[:, cols] = gate_d
            up_delta[:, cols] = up_d
            gate_acc[:, cols] += dot(rows_in, gate_d, 0, 0) * scale
            up_acc[:, cols] += dot(rows_in, up_d, 0, 0) * scale

            @pl.when(slab == slabs - 1)
            def _():
                for one in pair_sums(at):
                    one.start()

        blocks(body)

        @pl.when(slab < slabs - 1)
        def _():
            input_part(slab)

        @pl.when(slab > 0)
        def _():
            input_sum(slab - 1)

        @pl.when(slab == 1)
        def _():
            for one in sums_down:
                one.middle()

        @pl.when(slab == 2)
        def _():
            for one in sums_down:
                one.finish()

        @pl.when(slab == 4)
        def _():
            for one in sums_down:
                one.forward()

        @pl.when(slab == 6)
        def _():
            for one in sums_down:
                one.collect()
            for at in range(hidden // 128):
                values = fold(down_full[at * 128 : at * 128 + 128, :])
                down_squares[tp, at : at + 1, :] = row_sums(values)
            for by in range(1, tps):
                share(by).start()

        return carry

    lax.fori_loop(0, slabs, main_slab, 0)

    sums = [one for at in range(hidden // block) for one in pair_sums(at)]
    input_part(slabs - 1)
    for one in sums:
        one.middle()
    input_sum(slabs - 1)
    out_copy = pltpu.make_async_copy(input_fin, input_out, out_sem.at[0])
    out_copy.start()
    for one in sums:
        one.finish()
    for by in range(1, tps):
        shared(by).wait_recv()
    down_squares[tps] = sum(down_squares[at] for at in range(tps))
    down_rows_copy = pltpu.make_async_copy(down_squares.at[tps], down_rows_out, out_sem.at[1])
    down_rows_copy.start()
    for by in range(1, tps):
        share(by).wait_send()
    for one in sums:
        one.forward()

    for at in range(hidden // block):
        cols = pl.ds(at * block, block)
        for which, one in enumerate(sums[2 * at : 2 * at + 2]):
            one.collect()
            values = fold(one.full[:, cols])
            folded[which] = values if at == 0 else folded[which] + values
    blocks_in = width // 128
    for which in range(2):
        for at in range(blocks_in):
            row = which * blocks_in + at
            squares[0, row : row + 1, :] = row_sums(folded[which, at * 128 : at * 128 + 128, :])
    swap_squares = remote(
        squares.at[0], squares.at[1], square_sem.at[0], square_sem.at[1], {"fs": pair}
    )
    swap_squares.start()

    own_cot.wait_send()
    own_inputs.wait_send()
    out_copy.wait()

    def sent(origin, sems):
        place = cot.at[:, fs, :, lanes(origin)]
        return remote(place, place, sems.at[origin], own_sem.at[1], {"fs": pair})

    for origin in range(tps):

        @pl.when(jnp.logical_and(origin <= tp, tp < tps - 1))
        def _():
            sent(origin, line_right).wait_send()

        @pl.when(jnp.logical_and(origin >= tp, tp > 0))
        def _():
            sent(origin, line_left).wait_send()

        @pl.when(tp != origin)
        def _():
            sent(origin, pair_send).wait_send()

    remote(partial_in, partial_in, part_send.at[0], own_sem.at[1], {"fs": pair}).wait_send()
    for origin in range(tps):

        @pl.when(jnp.logical_and(origin <= tp, tp < tps - 1))
        def _():
            weight_line(origin, tp, 0, False).wait_send()

        @pl.when(jnp.logical_and(origin >= tp, tp > 0))
        def _():
            weight_line(origin, tp, 1, False).wait_send()

        @pl.when(tp != origin)
        def _():
            for at in range(4):
                weight_peer(origin, at).wait_send()

    for one in sums_down + sums:
        one.drain()
    swap_squares.wait()
    squares[2] = squares[0] + squares[1]
    rows_copy = pltpu.make_async_copy(squares.at[2], rows_out, out_sem.at[2])
    rows_copy.start()
    rows_copy.wait()
    down_rows_copy.wait()


def widen_kernel(grads, squares, down_squares, *outs):
    for source, target in zip(grads, outs[: len(grads)]):
        target[...] = source[...].astype(target.dtype)
    gate_rows, up_rows, down_rows = outs[len(grads) :]

    @pl.when(pl.program_id(0) == 0)
    def _():
        count = gate_rows.shape[0]
        gate_rows[...] = squares[:count, :]
        up_rows[...] = squares[count:, :]
        down_rows[...] = down_squares[...]


def widen(grads, kinds, squares, down_squares, steps):
    tall = [pl.BlockSpec((v.shape[0] // steps, v.shape[1]), lambda i: (i, 0)) for v in grads]
    whole = lambda shape: pl.BlockSpec(shape, lambda i: (0, 0))
    split = (squares.shape[0] // 2, squares.shape[1])
    small = [split, split, down_squares.shape]
    outs = pl.pallas_call(
        lambda *refs: widen_kernel(refs[: len(grads)], *refs[len(grads) :]),
        grid=(steps,),
        out_shape=[jax.ShapeDtypeStruct(v.shape, kind) for v, kind in zip(grads, kinds)]
        + [jax.ShapeDtypeStruct(shape, F32) for shape in small],
        in_specs=tall + [whole(squares.shape), whole(down_squares.shape)],
        out_specs=tall + [whole(shape) for shape in small],
        compiler_params=pltpu.CompilerParams(vmem_limit_bytes=62 * 2**20),
        name="widen",
    )(*grads, squares, down_squares)
    return [*outs[: len(grads)], *(v.reshape(-1) for v in outs[len(grads) :])]


def on_device(layer_input, cotangent, gate_pre, up_pre, gate_weight, up_weight, down_weight):
    tps, groups = lax.axis_size("tp"), lax.axis_size("rep")
    rows, width = layer_input.shape
    hidden = gate_pre.shape[1]
    side = math.gcd(rows, 128)
    slabs = rows // side
    block = math.gcd(hidden, 512)
    scale = 1.0 / math.sqrt(rows * groups * lax.axis_size("fs"))
    sizes = (tps, slabs, side, width, hidden, block, 1, scale)
    half, part = width // 2, width // 4
    rest = hidden // 2
    vmem = pltpu.VMEM
    dma = pltpu.SemaphoreType.DMA
    anywhere = pl.BlockSpec(memory_space=pl.ANY)
    pieces = lambda value: value.reshape(slabs, side, value.shape[1])
    both = lambda value: value.reshape(2, slabs, side, value.shape[1])
    sums_of = lambda n: [
        vmem((half, hidden), BF16),
        vmem((half, hidden), BF16),
        vmem((2, part, hidden), BF16),
        vmem((width, hidden), BF16),
    ]
    tokens = 2 * side
    input_grad, gate_grad, up_grad, down_grad, row_squares, down_squares = pl.pallas_call(
        functools.partial(kernel, sizes),
        out_shape=(
            jax.ShapeDtypeStruct((slabs, side, width), BF16),
            jax.ShapeDtypeStruct((width, hidden), BF16),
            jax.ShapeDtypeStruct((width, hidden), BF16),
            jax.ShapeDtypeStruct((hidden, width), BF16),
            jax.ShapeDtypeStruct((2 * width // 128, 128), F32),
            jax.ShapeDtypeStruct((hidden // 128, 128), F32),
        ),
        in_specs=[anywhere] * 7,
        out_specs=(anywhere,) * 6,
        scratch_shapes=[
            vmem((slabs, 2, side, tps * width), BF16),
            vmem((hidden, tps * width), BF16),
            vmem((slabs, 2, side, width), BF16),
            vmem((width, hidden), BF16),
            vmem((width, hidden), BF16),
            vmem((width, hidden), F32),
            vmem((width, hidden), F32),
            vmem((hidden, width), F32),
            vmem((2, 2, side, hidden), BF16),
            vmem((2, 2, side, hidden), BF16),
            vmem((tokens, hidden), BF16),
            vmem((tokens, hidden), BF16),
            vmem((slabs, 2, side, width), BF16),
            vmem((slabs, side, width), BF16),
            vmem((slabs, side, width), BF16),
        ]
        + sums_of(0)
        + sums_of(1)
        + [
            vmem((2, rest // 2, width), BF16),
            vmem((2, rest // 2, width), BF16),
            vmem((2, 2, rest // 4, width), BF16),
            vmem((hidden, width), BF16),
            vmem((2, width, 128), F32),
            vmem((3, 2 * width // 128, 128), F32),
            vmem((tps + 1, hidden // 128, 128), F32),
            dma((5,)),
            dma((2, 2)),
            dma((tps, slabs)),
            dma((tps,)),
            dma((tps,)),
            dma((tps,)),
            dma((tps, slabs)),
            dma((4,)),
            dma((tps,)),
            dma((2, tps)),
            dma((2, tps, 4)),
            dma((1,)),
            dma((slabs,)),
            dma((2, 2 + 2 * (hidden // block), 6)),
            dma((3,)),
            dma((2,)),
            dma((2, tps)),
        ],
        compiler_params=pltpu.CompilerParams(
            collective_id=0, has_side_effects=True, vmem_limit_bytes=62 * 2**20
        ),
        name="backward",
    )(
        pieces(layer_input),
        pieces(cotangent),
        both(gate_pre),
        both(up_pre),
        gate_weight,
        up_weight,
        down_weight,
    )
    input_grad = input_grad.reshape(rows, width)
    return tuple(
        widen(
            [input_grad, gate_grad, up_grad, down_grad],
            [BF16, F32, F32, F32],
            row_squares,
            down_squares,
            4,
        )
    )


def solution(mesh):
    return jax.shard_map(
        on_device,
        mesh=mesh,
        in_specs=(
            P(("rep", "fs"), "tp"),
            P(("rep", "fs"), "tp"),
            P("rep", "fs"),
            P("rep", "fs"),
            P("tp", "fs"),
            P("tp", "fs"),
            P("fs", "tp"),
        ),
        out_specs=(
            P(("rep", "fs"), "tp"),
            P("tp", "fs"),
            P("tp", "fs"),
            P("fs", "tp"),
            P("tp"),
            P("tp"),
            P("fs"),
        ),
        check_vma=False,
    )
```
